32 devices in a mesh: grp: 2 (over x), fs: 4 (over z), tp: 4 (over y, core).
Axes of the slice: x: 2, y: 2, z: 4, core: 2. Of those that a mesh axis runs over, the one named last changes fastest.
Arguments:
- stream: bfloat16 [2048, 2048], P(('grp', 'fs'), 'tp'), parts along dimension 0, may hold values from -80 to 80
- mixed: bfloat16 [2048, 2048], P(('grp', 'fs'), 'tp'), parts along dimension 0, may hold values from -6 to 6
- out_weight: bfloat16 [2048, 2048], P('fs', 'tp'), may hold values from -0.125 to 0.125
- norm_gain: bfloat16 [2048], P('tp'), may hold values from 0.099609375 to 1.8984375
- up_weight: bfloat16 [2048, 8192], P('fs', 'tp'), may hold values from -0.125 to 0.125
- down_weight: bfloat16 [8192, 2048], P('tp', 'fs'), may hold values from -0.09375 to 0.09375
Outputs:
- result: bfloat16 [2048, 2048], P(('grp', 'fs'), 'tp'), parts along dimension 0
The draws below stay inside these ranges and needn't reach their ends.
There are 2 independent parts, one for each index of `grp`. The reference program is written for one: setup_inputs(seed, part) draws one part's arguments, and reference() takes and returns one part's arrays. A program takes and returns all parts, laid end to end along the dimension named above; an argument that names none is the same for every part. Nothing has to cross between parts.
All inputs are finite; a program needn't handle non-finite values.
Results may differ from the reference program's by a relative error of at most 0.01.
Values may be sent and summed in bfloat16 or wider, within the bound.
A program may use at most 64 MiB of HBM per device.

```python
import jax
import jax.numpy as jnp
from jax import lax

D = 2048
FF = 8192
TOKENS = 1024


def draw_stream(key, part):
    base_key = jax.random.fold_in(key, 11)
    first, second, third = jax.random.split(base_key, 3)
    position = jnp.arange(D, dtype=jnp.float32) / max(D - 1, 1)
    column_scale = jnp.exp(position * jnp.log(4.0)) * jax.random.uniform(second, (D,), jnp.float32, 0.6, 1.4)
    row_scale = jnp.exp(jax.random.uniform(third, (TOKENS, 1), jnp.float32, jnp.log(0.5), jnp.log(2.0)))
    values = jnp.clip(jax.random.normal(first, (TOKENS, D), jnp.float32), -6.0, 6.0) * row_scale
    return (values * column_scale).astype(jnp.bfloat16)


def strengthened(drawn, key, source, target, parts, factor):
    owner, partner = [(jnp.arange(drawn.shape[dim]) // (drawn.shape[dim] // parts)).reshape([-1 if axis == dim else 1 for axis in range(drawn.ndim)]) for dim in (source, target)]
    chosen = jax.random.permutation(key, parts)[partner]
    strong = (owner == chosen) | (owner == (partner + parts // 2) % parts)
    return jnp.where(strong, factor * drawn, drawn)


def levels(key, extent, cuts, low, largest):
    factor_of = 1.0
    for dim, blocks in cuts:
        heights = jax.random.uniform(jax.random.fold_in(jax.random.fold_in(key, 6), dim), (blocks,), jnp.float32, low / len(cuts), largest / len(cuts))
        factor_of = factor_of * jnp.repeat(jnp.exp(heights), extent[dim] // blocks).reshape((-1,) + (1,) * (len(extent) - 1 - dim))
    return factor_of


def scatter_about(own_key, shape, deviation, limit, pieces=(), kind=jnp.bfloat16):
    entries = jax.random.normal(own_key, shape, jnp.float32) * deviation
    if len(pieces) > 0:
        entries = levels(own_key, shape, pieces, -0.22, 0.18) * entries
    return jnp.clip(entries, min=-limit, max=limit).astype(kind)


def noise_with(rng, extent, scale, bound, pieces, heavy, held_as=jnp.bfloat16):
    array = scale * jax.random.normal(rng, extent, jnp.float32)
    if pieces:
        array = array * levels(rng, extent, pieces, -0.22, 0.18)
    return jnp.clip(strengthened(array, jax.random.fold_in(rng, 3), *heavy), -bound, bound).astype(held_as)


def setup_inputs(seed: int = 0, part: int = 0) -> dict:
    keys = jax.random.split(jax.random.key(seed), 7)
    part_keys = jax.random.split(jax.random.fold_in(keys[6], part), 7)
    stream = draw_stream(jax.random.fold_in(jax.random.fold_in(keys[6], part), 71), part)
    mixed = scatter_about(part_keys[1], (TOKENS, D), 1.0, 6.0, ((0, 4), (1, 4)))
    out_weight = scatter_about(keys[2], (D, D), D ** -0.5, 0.125, ((0, 4), (1, 4)))
    norm_gain = jnp.clip(1.0 + 0.18 * jax.random.normal(keys[3], (D,), jnp.float32), 0.099609375, 1.8984375).astype(jnp.bfloat16)
    up_weight = scatter_about(keys[4], (D, FF), D ** -0.5, 0.125, ((0, 4), (1, 4)))
    down_weight = noise_with(keys[5], (FF, D), FF ** -0.5, 0.09375, ((0, 4), (1, 4)), (0, 1, 4, 2.0))
    return dict(stream=stream, mixed=mixed, out_weight=out_weight, norm_gain=norm_gain, up_weight=up_weight, down_weight=down_weight)


epsilon = 1e-06

def reference(stream, mixed, out_weight, norm_gain, up_weight, down_weight):
    projected = jnp.dot(mixed, out_weight, preferred_element_type=jnp.float32)
    resid = (stream.astype(jnp.float32) + projected).astype(jnp.bfloat16)
    widened = resid.astype(jnp.float32)
    energy = lax.optimization_barrier(jnp.mean(widened * widened, axis=-1, keepdims=True))
    normed = (widened * lax.rsqrt(energy + epsilon) * norm_gain.astype(jnp.float32)).astype(jnp.bfloat16)
    up_values = jnp.dot(normed, up_weight, preferred_element_type=jnp.float32)
    activated = jnp.square(jax.nn.relu(up_values)).astype(jnp.bfloat16)
    branch = jnp.dot(activated, down_weight, preferred_element_type=jnp.float32)
    return (widened + branch).astype(jnp.bfloat16)
```

```python
import functools

import jax
import jax.numpy as jnp
from jax import lax
from jax.experimental import pallas as pl
from jax.experimental.pallas import tpu as pltpu
from jax.sharding import PartitionSpec as P

epsilon = 1e-06


def fold_product(left, portion):
    return jnp.dot(left, portion, preferred_element_type=jnp.float32)


def gathered_body(stream, mixed, out_weight, norm_gain, up_weight, down_weight):
    mixed_whole = lax.all_gather(mixed, "tp", axis=1, tiled=True)
    projected = fold_product(mixed_whole, lax.all_gather(out_weight, "fs", axis=0, tiled=True))
    resid = (stream.astype(jnp.float32) + projected).astype(jnp.bfloat16)
    widened = resid.astype(jnp.float32)
    resid_whole, gain_whole = (
        lax.all_gather(resid, "tp", axis=1, tiled=True),
        lax.all_gather(norm_gain, "tp", axis=0, tiled=True),
    )
    stream_wide = resid_whole.astype(jnp.float32)
    energy = jnp.mean(stream_wide * stream_wide, axis=1, keepdims=True)
    normed_whole = (
        stream_wide * lax.rsqrt(energy + epsilon) * gain_whole.astype(jnp.float32)
    ).astype(jnp.bfloat16)
    up_full = lax.all_gather(up_weight, "fs", axis=0, tiled=True)
    up_values = jnp.dot(normed_whole, up_full, preferred_element_type=jnp.float32)
    activated = jnp.square(jax.nn.relu(up_values)).astype(jnp.bfloat16)
    partials = jnp.dot(
        activated,
        lax.all_gather(down_weight, "fs", axis=1, tiled=True),
        preferred_element_type=jnp.float32,
    )
    branch = lax.psum_scatter(partials, "tp", scatter_dimension=1, tiled=True)
    return (widened + branch).astype(jnp.bfloat16)


def spread_body(stream, mixed, out_weight, norm_gain, up_weight, down_weight):
    mixed_whole = lax.all_gather(mixed, "tp", axis=1, tiled=True)
    out_full = lax.all_gather(out_weight, "fs", axis=0, tiled=True)
    up_mine = lax.all_to_all(up_weight, "fs", split_axis=1, concat_axis=0, tiled=True)
    down_mine = lax.all_to_all(down_weight, "fs", split_axis=0, concat_axis=1, tiled=True)
    projected = jnp.dot(mixed_whole, out_full, preferred_element_type=jnp.float32)
    resid = (stream.astype(jnp.float32) + projected).astype(jnp.bfloat16)
    rows = lax.all_gather(resid, "fs", axis=0, tiled=True)
    whole = lax.all_gather(rows, "tp", axis=1, tiled=True).astype(jnp.float32)
    gain = lax.all_gather(norm_gain, "tp", axis=0, tiled=True).astype(jnp.float32)
    energy = jnp.mean(whole * whole, axis=1, keepdims=True)
    normed = (whole * lax.rsqrt(energy + epsilon) * gain).astype(jnp.bfloat16)
    up_values = jnp.dot(normed, up_mine, preferred_element_type=jnp.float32)
    activated = jnp.square(jax.nn.relu(up_values)).astype(jnp.bfloat16)
    partials = jnp.dot(activated, down_mine, preferred_element_type=jnp.float32).astype(jnp.bfloat16)
    columns = lax.psum_scatter(partials, "tp", scatter_dimension=1, tiled=True)
    branch = lax.psum_scatter(columns, "fs", scatter_dimension=0, tiled=True)
    return (resid.astype(jnp.float32) + branch.astype(jnp.float32)).astype(jnp.bfloat16)


MESH = pl.DeviceIdType.MESH


PARTS = dict(out=2, up=2, down=2, rows=2)


def slot_table(fs):
    table, count = {}, 0
    sizes = dict(mixed=3, gain=3, sum_c=fs * fs, sum_y=fs, sum_z=fs)
    for name, parts in PARTS.items():
        sizes[name + "_z"] = 2 * fs * parts
        for way in ("_x",) if name != "rows" else ("_y", "_c", "_d"):
            sizes[name + way] = fs * parts
    for name, size in sizes.items():
        table[name] = count
        count += size
    return table, count


def layer_kernel(
    fs, slots,
    stream_ref, mixed_ref, out_ref, gain_ref, up_ref, down_ref, result_ref,
    mixw, gains, wo, wup, wdn, rows, acts, kept, mine, send_c, got_c, send_y, got_y, send_z, got_z,
    held, send_sem, recv_sem, local_sem,
):
    f32, bf16 = jnp.float32, jnp.bfloat16
    g, i, j = lax.axis_index("grp"), lax.axis_index("fs"), lax.axis_index("tp")
    y, c = j // 2, j % 2
    jc = y * 2 + (1 - c)
    jy = (1 - y) * 2 + c
    jd = (1 - y) * 2 + (1 - c)
    half, width = wo.shape[2], wo.shape[3]

    core, across, diag, twin = (g, i, jc), (g, i, jy), (g, i, jd), (1 - g, i, j)
    both = jnp.logical_and

    def at(z):
        return (g, z, j)

    sent = []

    def copy(name, src, dst, target, sk, rk):
        return pltpu.make_async_remote_copy(
            src_ref=src, dst_ref=dst,
            send_sem=send_sem.at[slots[name] + sk], recv_sem=recv_sem.at[slots[name] + rk],
            device_id=target, device_id_type=MESH,
        )

    def send(name, src, dst, target, sk, rk, given=None):
        def go():
            copy(name, src, dst, target, sk, rk).start()

        if given is None:
            go()
        else:
            pl.when(given)(go)
        sent.append((name, sk, dst, given))

    def arrive(name, rk, dst):
        copy(name, dst, dst, core, rk, rk).wait_recv()

    def has(side, d):
        return i >= d if side == 0 else i + d < fs

    def source(side, d):
        return i - d if side == 0 else i + d

    def goes(side, d):
        return has(1 - side, d)

    def dest(side, d):
        return source(1 - side, d)

    def piece(ref, q, parts):
        size = ref.shape[0] // parts
        return ref.at[pl.ds(q * size, size), :]

    def relay_send(name, block_of, b, side, q, given):
        parts = PARTS[name]
        block = piece(block_of(b), q, parts)
        send(name + "_z", block, block, at(dest(side, 1)), (side * fs + b) * parts + q, b * parts + q, given)

    def relay(name, block_of, d, then):
        parts = PARTS[name]
        for q in range(parts):
            for side in range(2):
                b = source(side, d)
                given = has(side, d)

                @pl.when(given)
                def _():
                    arrive(name + "_z", b * parts + q, piece(block_of(b), q, parts))

                if d < fs - 1:
                    relay_send(name, block_of, b, side, q, both(given, goes(side, 1)))
                then(b, q, given)

    greeted = [core, across, diag, twin]
    barrier = pltpu.get_barrier_semaphore()
    for device in greeted:
        pl.semaphore_signal(barrier, inc=1, device_id=device, device_id_type=MESH)
    for s in range(1, fs):
        pl.semaphore_signal(barrier, inc=1, device_id=at(lax.rem(i + s, fs)), device_id_type=MESH)

    local = []

    def keep(src, dst):
        made = pltpu.make_async_copy(src, dst, local_sem.at[len(local)])
        made.start()
        local.append(made)

    def up_piece(owner, part):
        return up_ref.at[pl.ds(part * half, half), pl.ds(pl.multiple_of(owner * width, width), width)]

    def down_piece(owner, part):
        return down_ref.at[pl.ds(owner * 2 * half + part * half, half), :]

    for part in range(2):
        keep(out_ref.at[pl.ds(part * half, half), :], wo.at[i, part])
        keep(up_piece(i, part), wup.at[i, part])
        keep(down_piece(i, part), wdn.at[i, part])
    keep(mixed_ref, mixw.at[j])
    keep(stream_ref, held)
    gains[j] = gain_ref[...].astype(f32).reshape(1, width).astype(bf16)
    pl.semaphore_wait(barrier, len(greeted) + fs - 1)

    def exchange(name, piece_of, buffer, side, d, given):
        parts = PARTS[name]
        to = dest(side, d)
        for q in range(parts):
            send(
                name + "_z", piece(piece_of(to, g), q, parts), piece(buffer.at[i, g], q, parts), at(to),
                (side * fs + d) * parts + q, i * parts + q, both(given, goes(side, d)),
            )

    def take(name, buffer, b, given=None):
        parts = PARTS[name]
        for q in range(parts):
            block = piece(buffer.at[b, g], q, parts)

            def go():
                arrive(name + "_z", b * parts + q, block)

            if given is None:
                go()
            else:
                pl.when(given)(go)
            send(name + "_x", block, block, twin, b * parts + q, b * parts + q, given)

    def take_x(name, buffer, b):
        parts = PARTS[name]
        for q in range(parts):
            arrive(name + "_x", b * parts + q, piece(buffer.at[b, 1 - g], q, parts))

    def out_block(b):
        return wo.at[b, g]

    parts = PARTS["out"]
    own = out_ref.at[pl.ds(g * half, half), :]
    for q in range(parts):
        for side in range(2):
            send(
                "out_z", piece(own, q, parts), piece(wo.at[i, g], q, parts), at(dest(side, 1)),
                (side * fs + i) * parts + q, i * parts + q, goes(side, 1),
            )
    send("mixed", mixed_ref, mixw.at[j], across, 0, 0)
    send("mixed", mixed_ref, mixw.at[j], core, 1, 1)
    send("gain", gains.at[j], gains.at[j], across, 0, 0)
    send("gain", gains.at[j], gains.at[j], core, 1, 1)
    send("gain", gains.at[j], gains.at[j], diag, 2, 2)

    def ends(side, p):
        return i == p if side == 0 else i == fs - 1 - p

    def out_cross(b, q, given):
        block = piece(wo.at[b, g], q, PARTS["out"])
        n = b * PARTS["out"] + q
        send("out_x", block, block, twin, n, n, given)

    for d in range(fs):
        if d > 0:
            relay("out", out_block, d, out_cross)
        if d == 1:
            arrive("mixed", 0, mixw.at[jy])
            send("mixed", mixw.at[jy], mixw.at[jy], core, 2, 2)
        for side in range(2):
            for e in range(1, fs - d):
                exchange("up", up_piece, wup, side, e, ends(side, d))
    arrive("mixed", 1, mixw.at[jc])
    arrive("mixed", 2, mixw.at[jd])
    for made in local:
        made.wait()

    def whole(ref, k):
        return ref[k].reshape(2 * half, width)

    near = [(side, d) for d in range(1, fs) for side in range(2)]
    for side, d in near:
        @pl.when(has(side, d))
        def _():
            take_x("out", wo, source(side, d))

    total = held[...].astype(f32)
    for k in range(fs):
        total += jnp.dot(mixw[k], whole(wo, k), preferred_element_type=f32)
    rows[j, i] = total.astype(bf16)

    def rows_block(b):
        return rows.at[j, b]

    def rows_cross(b, q, given):
        parts = PARTS["rows"]
        block = piece(rows.at[j, b], q, parts)
        n = b * parts + q
        send("rows_y", block, block, across, n, n, given)
        send("rows_c", block, block, core, n, n, given)

    def rows_fetch(b):
        parts = PARTS["rows"]
        for q in range(parts):
            block = piece(rows.at[jy, b], q, parts)
            n = b * parts + q
            arrive("rows_y", n, block)
            copy("rows_d", block, block, core, n, n).start()

    def rows_sent(b, given):
        parts = PARTS["rows"]
        for q in range(parts):
            sent.append(("rows_d", b * parts + q, piece(rows.at[jy, b], q, parts), given))

    def rows_ready(b):
        parts = PARTS["rows"]
        for q in range(parts):
            n = b * parts + q
            arrive("rows_c", n, piece(rows.at[jc, b], q, parts))
            arrive("rows_d", n, piece(rows.at[jd, b], q, parts))

    for q in range(PARTS["rows"]):
        for side in range(2):
            relay_send("rows", rows_block, i, side, q, goes(side, 1))
        rows_cross(i, q, None)

    def down_issue(d):
        for side in range(2):
            for e in range(1, fs):
                for p in range(fs - e):
                    if max(p, 0 if e == 1 else e) == d:
                        exchange("down", down_piece, wdn, side, e, ends(side, p))

    down_issue(0)

    def hidden(t):
        wide = [rows[k, t].astype(f32) for k in range(rows.shape[0])]
        energy = sum(jnp.sum(w * w, axis=1, keepdims=True) for w in wide)
        scale = lax.rsqrt(energy * (1.0 / (len(wide) * width)) + epsilon)
        up = None
        for k, w in enumerate(wide):
            normed = (w * scale * gains[k].astype(f32)).astype(bf16)
            term = jnp.dot(normed, whole(wup, k), preferred_element_type=f32)
            up = term if up is None else up + term
        acts[t] = jnp.square(jnp.maximum(up, 0.0)).astype(bf16)

    for side, d in near:
        if d == 2 and side == 0:
            rows_fetch(i)
            rows_sent(i, None)
        take("up", wup, source(side, d), has(side, d))

    relay("rows", rows_block, 1, rows_cross)
    down_issue(1)
    arrive("gain", 0, gains.at[jy])
    arrive("gain", 1, gains.at[jc])
    arrive("gain", 2, gains.at[jd])
    for side, d in near:
        @pl.when(has(side, d))
        def _():
            take_x("up", wup, source(side, d))

    def fetch(side, d):
        given = has(side, d)
        pl.when(given)(lambda: rows_fetch(source(side, d)))
        rows_sent(source(side, d), given)

    def digest(side, d):
        @pl.when(has(side, d))
        def _():
            rows_ready(source(side, d))
            hidden(source(side, d))

    rows_ready(i)
    hidden(i)
    relay("rows", rows_block, 2, rows_cross)
    down_issue(2)
    fetch(0, 1)
    fetch(1, 1)
    digest(0, 1)
    relay("rows", rows_block, 3, rows_cross)
    down_issue(3)
    fetch(0, 2)
    fetch(1, 2)
    digest(1, 1)

    low = i < fs // 2
    m = jnp.where(low, i, fs - 1 - i)

    def column_of(n):
        f = jnp.where(m == 0, n, [1, 0, 2, 3][n])
        return jnp.where(low, f, fs - 1 - f)

    def token_of(n):
        f = jnp.where(m == 0, fs - 1 - n, [3, 2, 0, 1][n])
        return jnp.where(low, f, fs - 1 - f)

    fetch(0, 3)
    fetch(1, 3)
    digest(0, 2)
    digest(1, 2)
    digest(0, 3)
    digest(1, 3)

    def column(n):
        k = column_of(n)
        ck, yk = k % 2, k // 2
        w = whole(wdn, k)

        @pl.when(ck != c)
        def _():
            for s in range(fs):
                t = token_of(s)
                send_c[yk, t] = jnp.dot(acts[t], w, preferred_element_type=f32).astype(bf16)
                copy("sum_c", send_c.at[yk, t], got_c.at[yk, t], core, n * fs + s, n * fs + s).start()

        for s in range(fs):
            sent.append(("sum_c", n * fs + s, send_c.at[0, 0], ck != c))

        @pl.when(ck == c)
        def _():
            for s in range(fs):
                t = token_of(s)
                part = jnp.dot(acts[t], w, preferred_element_type=f32)
                arrive("sum_c", n * fs + s, got_c.at[yk, t])
                kept[t] = part + got_c[yk, t].astype(f32)

                @pl.when(yk != y)
                def _():
                    send_y[t] = kept[t].astype(bf16)
                    copy("sum_y", send_y.at[t], got_y.at[t], across, s, s).start()

                @pl.when(yk == y)
                def _():
                    mine[t] = kept[t]

        for s in range(fs):
            if n == 0:
                sent.append(("sum_y", s, send_y.at[0], None))

    def owned(n):
        @pl.when(column_of(n) == j)
        def _():
            for s in range(fs - 1):
                t = token_of(s)
                arrive("sum_y", s, got_y.at[t])
                send_z[t] = (mine[t] + got_y[t].astype(f32)).astype(bf16)
                copy("sum_z", send_z.at[t], got_z.at[i], at(t), t, i).start()

    take("down", wdn, column_of(1))
    column(0)
    take("down", wdn, column_of(2))
    take_x("down", wdn, column_of(1))
    column(1)
    take("down", wdn, column_of(3))
    owned(0)
    take_x("down", wdn, column_of(2))
    column(2)
    owned(1)
    take_x("down", wdn, column_of(3))
    column(3)
    owned(2)
    owned(3)
    for s in range(fs - 1):
        sent.append(("sum_z", token_of(s), send_z.at[0], None))
    arrive("sum_y", fs - 1, got_y.at[i])
    branch = mine[i] + got_y[i].astype(f32)
    for s in range(fs - 2, -1, -1):
        b = token_of(s)
        arrive("sum_z", b, got_z.at[b])
        branch += got_z[b].astype(f32)
    held[...] = (rows[j, i].astype(f32) + branch).astype(bf16)
    out_copy = pltpu.make_async_copy(held, result_ref, local_sem.at[0])
    out_copy.start()
    for name, sk, block, given in sent:
        def done():
            copy(name, block, block, core, sk, sk).wait_send()

        if given is None:
            done()
        else:
            pl.when(given)(done)
    out_copy.wait()


def kernel_body(fs, tp, stream, mixed, out_weight, norm_gain, up_weight, down_weight):
    tokens, width = stream.shape
    half = out_weight.shape[0] // 2
    slots, count = slot_table(fs)
    vmem, anywhere = pl.BlockSpec(memory_space=pltpu.VMEM), pl.BlockSpec(memory_space=pl.ANY)
    weights = pltpu.VMEM((fs, 2, half, width), jnp.bfloat16)
    blocks = pltpu.VMEM((fs, tokens, width), jnp.bfloat16)
    columns = pltpu.VMEM((2, fs, tokens, width), jnp.bfloat16)
    sums = pltpu.VMEM((fs, tokens, width), jnp.float32)
    return pl.pallas_call(
        functools.partial(layer_kernel, fs, slots),
        out_shape=jax.ShapeDtypeStruct((tokens, width), jnp.bfloat16),
        in_specs=[anywhere, anywhere, anywhere, vmem, anywhere, anywhere],
        out_specs=anywhere,
        scratch_shapes=[
            pltpu.VMEM((tp, tokens, width), jnp.bfloat16),
            pltpu.VMEM((tp, 1, width), jnp.bfloat16),
            weights, weights, weights,
            pltpu.VMEM((tp, fs, tokens, width), jnp.bfloat16),
            blocks,
            sums, sums,
            columns, columns, blocks, blocks, blocks, blocks,
            pltpu.VMEM((tokens, width), jnp.bfloat16),
            pltpu.SemaphoreType.DMA((count,)),
            pltpu.SemaphoreType.DMA((count,)),
            pltpu.SemaphoreType.DMA((8,)),
        ],
        compiler_params=pltpu.CompilerParams(
            collective_id=0, has_side_effects=True, vmem_limit_bytes=56 * 1024 * 1024
        ),
    )(stream, mixed, out_weight, norm_gain, up_weight, down_weight)


def solution(mesh):
    placed = (
        P(("grp", "fs"), "tp"),
        P(("grp", "fs"), "tp"),
        P("fs", "tp"),
        P("tp"),
        P("fs", "tp"),
        P("tp", "fs"),
    )
    fs, tp = mesh.shape["fs"], mesh.shape["tp"]

    def call(stream, mixed, out_weight, norm_gain, up_weight, down_weight):
        width, hidden = up_weight.shape
        tokens = stream.shape[0] // mesh.shape["grp"]
        moved_weights = 2 * width * hidden // tp
        moved_rows = 2 * tokens * width + 2 * width * hidden // (tp * fs)
        aligned = fs == tp == 4 and (width // tp) % 256 == 0 and (tokens // fs) % 16 == 0
        aligned = aligned and hidden == tp * width
        body = spread_body if moved_rows < moved_weights else gathered_body
        if aligned and moved_rows < moved_weights:
            body = functools.partial(kernel_body, fs, tp)
        return sharded(body)(stream, mixed, out_weight, norm_gain, up_weight, down_weight)

    def sharded(body):
        return jax.shard_map(
            body, mesh=mesh, in_specs=placed, out_specs=P(("grp", "fs"), "tp"), check_vma=False
        )

    return call
```

```python
import functools

import jax
import jax.numpy as jnp
from jax import lax
from jax.experimental import pallas as pl
from jax.experimental.pallas import tpu as pltpu
from jax.sharding import PartitionSpec as P

epsilon = 1e-06


def fold_product(left, portion):
    return jnp.dot(left, portion, preferred_element_type=jnp.float32)


def gathered_body(stream, mixed, out_weight, norm_gain, up_weight, down_weight):
    mixed_whole = lax.all_gather(mixed, "tp", axis=1, tiled=True)
    projected = fold_product(mixed_whole, lax.all_gather(out_weight, "fs", axis=0, tiled=True))
    resid = (stream.astype(jnp.float32) + projected).astype(jnp.bfloat16)
    widened = resid.astype(jnp.float32)
    resid_whole, gain_whole = (
        lax.all_gather(resid, "tp", axis=1, tiled=True),
        lax.all_gather(norm_gain, "tp", axis=0, tiled=True),
    )
    stream_wide = resid_whole.astype(jnp.float32)
    energy = jnp.mean(stream_wide * stream_wide, axis=1, keepdims=True)
    normed_whole = (
        stream_wide * lax.rsqrt(energy + epsilon) * gain_whole.astype(jnp.float32)
    ).astype(jnp.bfloat16)
    up_full = lax.all_gather(up_weight, "fs", axis=0, tiled=True)
    up_values = jnp.dot(normed_whole, up_full, preferred_element_type=jnp.float32)
    activated = jnp.square(jax.nn.relu(up_values)).astype(jnp.bfloat16)
    partials = jnp.dot(
        activated,
        lax.all_gather(down_weight, "fs", axis=1, tiled=True),
        preferred_element_type=jnp.float32,
    )
    branch = lax.psum_scatter(partials, "tp", scatter_dimension=1, tiled=True)
    return (widened + branch).astype(jnp.bfloat16)


def spread_body(stream, mixed, out_weight, norm_gain, up_weight, down_weight):
    mixed_whole = lax.all_gather(mixed, "tp", axis=1, tiled=True)
    out_full = lax.all_gather(out_weight, "fs", axis=0, tiled=True)
    up_mine = lax.all_to_all(up_weight, "fs", split_axis=1, concat_axis=0, tiled=True)
    down_mine = lax.all_to_all(down_weight, "fs", split_axis=0, concat_axis=1, tiled=True)
    projected = jnp.dot(mixed_whole, out_full, preferred_element_type=jnp.float32)
    resid = (stream.astype(jnp.float32) + projected).astype(jnp.bfloat16)
    rows = lax.all_gather(resid, "fs", axis=0, tiled=True)
    whole = lax.all_gather(rows, "tp", axis=1, tiled=True).astype(jnp.float32)
    gain = lax.all_gather(norm_gain, "tp", axis=0, tiled=True).astype(jnp.float32)
    energy = jnp.mean(whole * whole, axis=1, keepdims=True)
    normed = (whole * lax.rsqrt(energy + epsilon) * gain).astype(jnp.bfloat16)
    up_values = jnp.dot(normed, up_mine, preferred_element_type=jnp.float32)
    activated = jnp.square(jax.nn.relu(up_values)).astype(jnp.bfloat16)
    partials = jnp.dot(activated, down_mine, preferred_element_type=jnp.float32).astype(jnp.bfloat16)
    columns = lax.psum_scatter(partials, "tp", scatter_dimension=1, tiled=True)
    branch = lax.psum_scatter(columns, "fs", scatter_dimension=0, tiled=True)
    return (resid.astype(jnp.float32) + branch.astype(jnp.float32)).astype(jnp.bfloat16)


MESH = pl.DeviceIdType.MESH


PARTS = dict(out=2, up=2, down=2, rows=2)

SCRIPTS = {
    (0, 0): [
        10, 11, 900, 210, 310, 211, 1000, 311, 120, 320, 131, 321, 430, 121, 130, 610, 110, 530, 330, 111,
        331, 431, 1100, 620, 630, 1800, 1310, 1400, 1311, 531, 1600, 1410, 410, 411, 1510, 1610, 420, 1511,
        1611, 1520, 230, 1601, 421, 231, 220, 221, 1620, 1621, 1521, 1530, 1200, 710, 720, 730, 1700, 1900,
        1710, 1910, 1720, 1920, 1531, 1999, 2020, 830, 2023, 2010, 2013, 1630, 2123, 1999, 2000, 1999, 2120,
        2199, 2003, 2110, 520, 2199, 2099, 2099, 2199, 2099, 2100, 521, 1631, 1730, 2199, 1930, 2030, 2130,
        2033, 2133, 510, 820, 2032, 2022, 2012, 2113, 2103, 2199, 511, 2132, 2122, 2002, 2299, 2112, 2102,
        810, 2011, 2031, 2021, 2001, 2131, 2121, 2111, 2230, 2101, 2220, 2210, 2299, 2300,
    ],
    (0, 1): [
        900, 10, 11, 211, 210, 1000, 230, 130, 310, 321, 320, 311, 120, 330, 121, 620, 231, 331, 131, 430,
        110, 431, 1100, 610, 630, 1800, 1310, 1400, 1311, 421, 420, 1410, 1600, 111, 1510, 720, 410, 411,
        1601, 1511, 1610, 1520, 1200, 710, 730, 1700, 1900, 1999, 1999, 1999, 2000, 2099, 2099, 2099, 1521,
        1611, 1710, 2199, 1910, 1620, 2010, 530, 1530, 1621, 1720, 531, 1920, 2100, 2199, 2020, 1630, 1531,
        2120, 2110, 830, 2003, 2023, 2199, 2013, 2103, 221, 220, 510, 2113, 1631, 1730, 1930, 511, 2033, 2123,
        2030, 2130, 520, 810, 2031, 2001, 2021, 2199, 2133, 2199, 2131, 2101, 2011, 2299, 2121, 521, 2111,
        820, 2022, 2032, 2002, 2012, 2132, 2102, 2122, 2230, 2112, 2220, 2210, 2299, 2300,
    ],
    (1, 0): [
        20, 21, 0, 900, 1, 300, 320, 1000, 301, 321, 330, 500, 130, 331, 131, 501, 430, 100, 431, 101, 600,
        620, 630, 1100, 1800, 1300, 1400, 1301, 1320, 1321, 1410, 1610, 1611, 120, 1520, 400, 121, 401, 1521,
        1620, 1500, 420, 1621, 1501, 1600, 1530, 220, 1601, 1531, 1630, 1631, 221, 421, 520, 730, 1200, 1710,
        700, 720, 1910, 1700, 1900, 230, 521, 1720, 1920, 1730, 1930, 800, 820, 2030, 2031, 2010, 231, 200,
        201, 2020, 2110, 1999, 2011, 1999, 2130, 2199, 2032, 2199, 2111, 2012, 2021, 2120, 2000, 2121, 2131,
        1999, 2099, 2132, 2001, 2100, 2002, 2022, 2099, 2199, 2199, 2112, 2122, 2101, 2099, 2200, 2102, 531,
        530, 830, 2199, 2023, 2033, 2013, 2003, 2133, 2113, 2123, 2299, 2103, 2230, 2220, 2299, 2300,
    ],
    (1, 1): [
        20, 900, 0, 1, 21, 300, 320, 1000, 301, 321, 330, 331, 1100, 500, 501, 430, 100, 431, 600, 101, 620,
        630, 1800, 1320, 1400, 1301, 1321, 1410, 1610, 120, 1300, 1520, 400, 130, 1611, 1521, 1500, 420, 1620,
        1501, 421, 401, 1621, 1600, 1530, 131, 1601, 121, 1630, 730, 220, 1531, 1200, 700, 720, 1710, 1910,
        1700, 1900, 1720, 1920, 1631, 1999, 2001, 800, 221, 2000, 2021, 1730, 2099, 2100, 1930, 2099, 230,
        1999, 2199, 2121, 200, 2031, 2199, 2101, 2020, 2030, 2199, 2011, 2131, 2199, 1999, 2010, 2130, 2099,
        2111, 201, 231, 530, 531, 520, 521, 830, 2003, 2023, 2033, 2120, 2199, 2110, 2103, 2123, 2013, 2299,
        2133, 2113, 820, 2032, 2002, 2022, 2012, 2102, 2122, 2132, 2299, 2112, 2230, 2200, 2220, 2300,
    ],
}


GROUPS = dict(z=0, x=1, mixed=1, y=2, c=2, d=2, sum_c=3, sum_y=4, sum_a=5, sum_z=5, gain=6)


def slot_table(fs):
    table, count = {}, 0
    sizes = dict(mixed=3, gain=1, sum_c=2 * fs, sum_y=fs, sum_a=2, sum_z=2, rows_c=fs, rows_d=fs)
    for name, parts in PARTS.items():
        sizes[name + "_z"] = fs * parts
        if name == "rows":
            sizes["rows_y"] = fs * parts
        else:
            sizes[name + "_x"] = fs
    for name, size in sizes.items():
        table[name] = count
        count += size
    return table, count


LETTERS, TWO, ONE = "AUDaudxvzmnlgBybrwPHCFOE", "AUDaudBbrCF", "xvzywHO"


def unpack(code):
    kind, rest = LETTERS[code // 100], code % 100
    if rest == 99:
        return kind, None
    count = 2 if kind in TWO else 1 if kind in ONE else 0
    return kind, [rest // 10, rest % 10][:count]


def segments(script):
    parts, steps = [[]], []
    for token in map(unpack, script):
        if token[0] in "PHCFOE":
            steps.append(token)
            parts.append([])
        else:
            parts[-1].append(token)
    return parts, steps


def layer_kernel(
    fs, slots,
    stream_ref, mixed_ref, out_ref, gain_ref, up_ref, down_ref, result_ref,
    mixw, gains, wo, wup, wdn, rows, acts, kept, send_c, got_c, send_y, got_y, send_z, got_a, got_z,
    held, send_sem, recv_sem, local_sem,
):
    f32, bf16 = jnp.float32, jnp.bfloat16
    g, i, j = lax.axis_index("grp"), lax.axis_index("fs"), lax.axis_index("tp")
    y, c = j // 2, j % 2
    jc = y * 2 + (1 - c)
    jy = (1 - y) * 2 + c
    jd = (1 - y) * 2 + (1 - c)
    half, width = wo.shape[2], wo.shape[3]

    low = i < fs // 2
    v = jnp.where(low, i, fs - 1 - i)
    yr = jnp.where(low, y, 1 - y)
    cr = jnp.where(low, c, 1 - c)

    def real(w):
        return jnp.where(low, w, fs - 1 - w)

    core, across, diag, twin = (g, i, jc), (g, i, jy), (g, i, jd), (1 - g, i, j)
    both = jnp.logical_and

    def at(w):
        return (g, real(w), j)

    def group(name):
        return GROUPS[name] if name in GROUPS else GROUPS[name.split("_")[1]]

    def copy(name, src, dst, target, rk):
        return pltpu.make_async_remote_copy(
            src_ref=src, dst_ref=dst,
            send_sem=send_sem.at[group(name)], recv_sem=recv_sem.at[slots[name] + rk],
            device_id=target, device_id_type=MESH,
        )

    def send(name, src, dst, target, rk):
        copy(name, src, dst, target, rk).start()

    def arrive(name, rk, dst):
        copy(name, dst, dst, core, rk).wait_recv()

    barrier = pltpu.get_barrier_semaphore()
    greeted = [core, across, diag, twin]
    for device in greeted:
        pl.semaphore_signal(barrier, inc=1, device_id=device, device_id_type=MESH)
    for s in range(1, fs):
        pl.semaphore_signal(barrier, inc=1, device_id=(g, lax.rem(i + s, fs), j), device_id_type=MESH)

    def keep(src, dst):
        pltpu.make_async_copy(src, dst, local_sem.at[0]).start()

    def up_piece(owner, part):
        return up_ref.at[pl.ds(part * half, half), pl.ds(pl.multiple_of(owner * width, width), width)]

    def down_piece(owner, part):
        return down_ref.at[pl.ds(owner * 2 * half + part * half, half), :]

    for part in range(2):
        keep(out_ref.at[pl.ds(part * half, half), :], wo.at[i, part])
        keep(up_piece(i, part), wup.at[i, part])
        keep(down_piece(i, part), wdn.at[i, part])
    keep(mixed_ref, mixw.at[j])
    keep(stream_ref, held)
    gains[j] = gain_ref[...].astype(f32).reshape(1, width).astype(bf16)
    pl.semaphore_wait(barrier, len(greeted) + fs - 1)

    def piece(name, ref, q):
        size = ref.shape[0] // PARTS[name]
        return ref.at[pl.ds(q * size, size), :]

    def block_of(name, w):
        if name == "rows":
            return rows.at[j, real(w)]
        return dict(out=wo, up=wup, down=wdn)[name].at[real(w), g]

    def slot(name, b, q):
        return real(b) * PARTS[name] + q

    def pass_on(name, b, q, to):
        block = piece(name, block_of(name, b), q)
        send(name + "_z", block, block, at(to), slot(name, b, q))

    def crossing(b, q):
        block = piece("rows", block_of("rows", b), q)
        send("rows_y", block, block, across, slot("rows", b, q))
        send("rows_c", block, block, core, real(b))

    def twin_copy(name, b, q):
        block = piece(name, block_of(name, b), q)
        send(name + "_x", block, block, twin, real(b))

    def act(own, token):
        kind, args = token
        if kind in "AUD":
            w, q = args
            name = dict(A="out", U="up", D="down")[kind]
            to = real(w)
            source = dict(
                A=out_ref.at[pl.ds(g * half, half), :], U=up_piece(to, g), D=down_piece(to, g)
            )[kind]
            send(
                name + "_z", piece(name, source, q), piece(name, block_of(name, own), q), at(w),
                slot(name, own, q),
            )
        elif kind in "aud":
            b, q = args
            name = dict(a="out", u="up", d="down")[kind]
            arrive(name + "_z", slot(name, b, q), piece(name, block_of(name, b), q))
            if kind == "a":
                to = own + 1 if b < own else own - 1
                if to >= 0:
                    pass_on(name, b, q, to)
            twin_copy(name, b, q)
        elif kind in "xvz":
            (b,) = args
            name, buffer = dict(x=("out", wo), v=("up", wup), z=("down", wdn))[kind]
            arrive(name + "_x", real(b), buffer.at[real(b), 1 - g])
        elif kind == "m":
            send("mixed", mixed_ref, mixw.at[j], across, 0)
            send("mixed", mixed_ref, mixw.at[j], core, 1)
            for target in (across, core, diag):
                send("gain", gains.at[j], gains.at[j], target, 0)
        elif kind == "n":
            arrive("mixed", 0, mixw.at[jy])
            send("mixed", mixw.at[jy], mixw.at[jy], core, 2)
        elif kind == "l":
            arrive("mixed", 1, mixw.at[jc])
            arrive("mixed", 2, mixw.at[jd])
        elif kind == "g":
            arrive("gain", 0, gains.at[pl.ds(0, 3)])
        elif kind == "B":
            w, q = args
            pass_on("rows", own, q, w)
        elif kind == "y":
            (q,) = args
            crossing(own, q)
        elif kind == "b":
            b, q = args
            arrive("rows_z", slot("rows", b, q), piece("rows", block_of("rows", b), q))
            to = own + 1 if b < own else own - 1
            if to >= 0:
                pass_on("rows", b, q, to)
            crossing(b, q)
        elif kind == "r":
            b, q = args
            block = piece("rows", rows.at[jy, real(b)], q)
            arrive("rows_y", slot("rows", b, q), block)
            send("rows_d", block, block, core, real(b))
        elif kind == "w":
            (b,) = args
            arrive("rows_c", real(b), rows.at[jc, real(b)])
            arrive("rows_d", real(b), rows.at[jd, real(b)])

    def whole(ref, k):
        return ref[k].reshape(2 * half, width)

    kinds = [(a, b) for a in range(2) for b in range(2)]
    plans = [segments(SCRIPTS[kind]) for kind in kinds]

    def pick(values):
        lower = values[0] if values[0] == values[1] else jnp.where(yr == 0, values[0], values[1])
        upper = values[2] if values[2] == values[3] else jnp.where(yr == 0, values[2], values[3])
        if list(values[:2]) == list(values[2:]):
            return lower
        return jnp.where(v == 0, lower, upper)

    def project():
        pltpu.make_async_copy(send_c, got_c, local_sem.at[0]).wait()
        total = held[...].astype(f32)
        for k in range(fs):
            total += jnp.dot(mixw[k], whole(wo, k), preferred_element_type=f32)
        rows[j, i] = total.astype(bf16)

    def hidden(t):
        z = real(t)
        wide = [rows[k, z].astype(f32) for k in range(rows.shape[0])]
        energy = sum(jnp.sum(w * w, axis=1, keepdims=True) for w in wide)
        scale = lax.rsqrt(energy * (1.0 / (len(wide) * width)) + epsilon)
        up = None
        for k, w in enumerate(wide):
            normed = (w * scale * gains[k].astype(f32)).astype(bf16)
            term = jnp.dot(normed, whole(wup, k), preferred_element_type=f32)
            up = term if up is None else up + term
        acts[t] = jnp.square(jnp.maximum(up, 0.0)).astype(bf16)

    def column(t, k):
        p = k // 2
        part = jnp.dot(acts[t], whole(wdn, real(k)), preferred_element_type=f32)

        @pl.when(k % 2 != cr)
        def _():
            send_c[p, t] = part.astype(bf16)
            copy("sum_c", send_c.at[p, t], got_c.at[p, t], core, p * fs + t).start()

        @pl.when(k % 2 == cr)
        def _():
            kept[p, t] = part

    def fold(t, k):
        p = k // 2

        @pl.when(k % 2 == cr)
        def _():
            arrive("sum_c", p * fs + t, got_c.at[p, t])
            kept[p, t] = kept[p, t] + got_c[p, t].astype(f32)

            @pl.when(p != yr)
            def _():
                send_y[t] = kept[p, t].astype(bf16)
                copy("sum_y", send_y.at[t], got_y.at[t], across, t).start()

    def offer(t):
        arrive("sum_y", t, got_y.at[t])
        joined = both(v == 1, t >= fs // 2)
        first = both(v == 0, t >= fs // 2)
        kept[yr, t] = kept[yr, t] + got_y[t].astype(f32)

        @pl.when(joined)
        def _():
            arrive("sum_a", t - fs // 2, got_a.at[t - fs // 2])
            send_z[t] = (kept[yr, t] + got_a[t - fs // 2].astype(f32)).astype(bf16)
            copy("sum_z", send_z.at[t], got_z.at[1], at(t), 1).start()

        @pl.when(first)
        def _():
            send_z[t] = kept[yr, t].astype(bf16)
            copy("sum_a", send_z.at[t], got_a.at[t - fs // 2], at(1), t - fs // 2).start()

        @pl.when(t < fs // 2)
        def _():
            send_z[t] = kept[yr, t].astype(bf16)
            copy("sum_z", send_z.at[t], got_z.at[0], at(t), 0).start()

    def finish():
        arrive("sum_y", v, got_y.at[v])
        branch = kept[yr, v] + got_y[v].astype(f32)
        for n in range(2):
            arrive("sum_z", n, got_z.at[n])
            branch += got_z[n].astype(f32)
        held[...] = (rows[j, i].astype(f32) + branch).astype(bf16)

    mine = [v == own for own in range(2)]
    exact = [[both(mine[own], yr == b) for b in range(2)] for own in range(2)]
    for n in range(len(plans[0][0])):
        for own in range(2):
            lists = [plans[2 * own + b][0][n] for b in range(2)]
            if lists[0] == lists[1]:
                if lists[0]:
                    @pl.when(mine[own])
                    def _():
                        for token in lists[0]:
                            act(own, token)
            else:
                for b in range(2):
                    if lists[b]:
                        given = exact[own][b]

                        @pl.when(given)
                        def _():
                            for token in lists[b]:
                                act(own, token)
        if n < len(plans[0][1]):
            steps = [plan[1][n] for plan in plans]
            kind = steps[0][0]
            taken = [step[1] is not None for step in steps]
            if not any(taken):
                continue
            default = steps[taken.index(True)]
            choices = [step[1] if used else default[1] for step, used in zip(steps, taken)]
            args = [pick(list(values)) for values in zip(*choices)]
            run = dict(P=project, H=hidden, C=column, F=fold, O=offer, E=finish)[kind]
            if all(taken):
                run(*args)
            else:
                here = functools.reduce(
                    jnp.logical_or, [one for one, used in zip(exact[0] + exact[1], taken) if used]
                )
                pl.when(here)(functools.partial(run, *args))

    out_copy = pltpu.make_async_copy(held, result_ref, local_sem.at[1])
    out_copy.start()

    def drain(name, total):
        copy(name, total, total, core, 0).wait_send()

    @pl.when(v == 0)
    def _():
        drain("out_z", got_c)

    @pl.when(v == 1)
    def _():
        drain("out_z", rows)

    drain("mixed", rows.at[pl.ds(0, 3)])
    drain("rows_y", rows.at[pl.ds(0, 3)])
    drain("sum_c", got_c)
    drain("sum_y", got_y)
    drain("sum_z", send_z.at[pl.ds(0, 3)])
    drain("gain", gains.at[pl.ds(0, 3)])
    out_copy.wait()


def kernel_body(fs, tp, stream, mixed, out_weight, norm_gain, up_weight, down_weight):
    tokens, width = stream.shape
    half = out_weight.shape[0] // 2
    slots, count = slot_table(fs)
    vmem, anywhere = pl.BlockSpec(memory_space=pltpu.VMEM), pl.BlockSpec(memory_space=pl.ANY)
    weights = pltpu.VMEM((fs, 2, half, width), jnp.bfloat16)
    blocks = pltpu.VMEM((fs, tokens, width), jnp.bfloat16)
    columns = pltpu.VMEM((2, fs, tokens, width), jnp.bfloat16)
    pair = pltpu.VMEM((2, tokens, width), jnp.bfloat16)
    return pl.pallas_call(
        functools.partial(layer_kernel, fs, slots),
        out_shape=jax.ShapeDtypeStruct((tokens, width), jnp.bfloat16),
        in_specs=[anywhere, anywhere, anywhere, vmem, anywhere, anywhere],
        out_specs=anywhere,
        scratch_shapes=[
            pltpu.VMEM((tp, tokens, width), jnp.bfloat16),
            pltpu.VMEM((tp, 1, width), jnp.bfloat16),
            weights, weights, weights,
            pltpu.VMEM((tp, fs, tokens, width), jnp.bfloat16),
            blocks,
            pltpu.VMEM((2, fs, tokens, width), jnp.float32),
            columns, columns, blocks, blocks, blocks, pair, pair,
            pltpu.VMEM((tokens, width), jnp.bfloat16),
            pltpu.SemaphoreType.DMA((7,)),
            pltpu.SemaphoreType.DMA((count,)),
            pltpu.SemaphoreType.DMA((2,)),
        ],
        compiler_params=pltpu.CompilerParams(
            collective_id=0, has_side_effects=True, vmem_limit_bytes=56 * 1024 * 1024
        ),
    )(stream, mixed, out_weight, norm_gain, up_weight, down_weight)


def solution(mesh):
    placed = (
        P(("grp", "fs"), "tp"),
        P(("grp", "fs"), "tp"),
        P("fs", "tp"),
        P("tp"),
        P("fs", "tp"),
        P("tp", "fs"),
    )
    fs, tp = mesh.shape["fs"], mesh.shape["tp"]

    def call(stream, mixed, out_weight, norm_gain, up_weight, down_weight):
        width, hidden = up_weight.shape
        tokens = stream.shape[0] // mesh.shape["grp"]
        moved_weights = 2 * width * hidden // tp
        moved_rows = 2 * tokens * width + 2 * width * hidden // (tp * fs)
        aligned = fs == tp == 4 and (width // tp) % 256 == 0 and (tokens // fs) % 16 == 0
        aligned = aligned and hidden == tp * width
        body = spread_body if moved_rows < moved_weights else gathered_body
        if aligned and moved_rows < moved_weights:
            body = functools.partial(kernel_body, fs, tp)
        return sharded(body)(stream, mixed, out_weight, norm_gain, up_weight, down_weight)

    def sharded(body):
        return jax.shard_map(
            body, mesh=mesh, in_specs=placed, out_specs=P(("grp", "fs"), "tp"), check_vma=False
        )

    return call
```

```python
import functools

import jax
import jax.numpy as jnp
from jax import lax
from jax.experimental import pallas as pl
from jax.experimental.pallas import tpu as pltpu
from jax.sharding import PartitionSpec as P

epsilon = 1e-06


def fold_product(left, portion):
    return jnp.dot(left, portion, preferred_element_type=jnp.float32)


def gathered_body(stream, mixed, out_weight, norm_gain, up_weight, down_weight):
    mixed_whole = lax.all_gather(mixed, "tp", axis=1, tiled=True)
    projected = fold_product(mixed_whole, lax.all_gather(out_weight, "fs", axis=0, tiled=True))
    resid = (stream.astype(jnp.float32) + projected).astype(jnp.bfloat16)
    widened = resid.astype(jnp.float32)
    resid_whole, gain_whole = (
        lax.all_gather(resid, "tp", axis=1, tiled=True),
        lax.all_gather(norm_gain, "tp", axis=0, tiled=True),
    )
    stream_wide = resid_whole.astype(jnp.float32)
    energy = jnp.mean(stream_wide * stream_wide, axis=1, keepdims=True)
    normed_whole = (
        stream_wide * lax.rsqrt(energy + epsilon) * gain_whole.astype(jnp.float32)
    ).astype(jnp.bfloat16)
    up_full = lax.all_gather(up_weight, "fs", axis=0, tiled=True)
    up_values = jnp.dot(normed_whole, up_full, preferred_element_type=jnp.float32)
    activated = jnp.square(jax.nn.relu(up_values)).astype(jnp.bfloat16)
    partials = jnp.dot(
        activated,
        lax.all_gather(down_weight, "fs", axis=1, tiled=True),
        preferred_element_type=jnp.float32,
    )
    branch = lax.psum_scatter(partials, "tp", scatter_dimension=1, tiled=True)
    return (widened + branch).astype(jnp.bfloat16)


def spread_body(stream, mixed, out_weight, norm_gain, up_weight, down_weight):
    mixed_whole = lax.all_gather(mixed, "tp", axis=1, tiled=True)
    out_full = lax.all_gather(out_weight, "fs", axis=0, tiled=True)
    up_mine = lax.all_to_all(up_weight, "fs", split_axis=1, concat_axis=0, tiled=True)
    down_mine = lax.all_to_all(down_weight, "fs", split_axis=0, concat_axis=1, tiled=True)
    projected = jnp.dot(mixed_whole, out_full, preferred_element_type=jnp.float32)
    resid = (stream.astype(jnp.float32) + projected).astype(jnp.bfloat16)
    rows = lax.all_gather(resid, "fs", axis=0, tiled=True)
    whole = lax.all_gather(rows, "tp", axis=1, tiled=True).astype(jnp.float32)
    gain = lax.all_gather(norm_gain, "tp", axis=0, tiled=True).astype(jnp.float32)
    energy = jnp.mean(whole * whole, axis=1, keepdims=True)
    normed = (whole * lax.rsqrt(energy + epsilon) * gain).astype(jnp.bfloat16)
    up_values = jnp.dot(normed, up_mine, preferred_element_type=jnp.float32)
    activated = jnp.square(jax.nn.relu(up_values)).astype(jnp.bfloat16)
    partials = jnp.dot(activated, down_mine, preferred_element_type=jnp.float32).astype(jnp.bfloat16)
    columns = lax.psum_scatter(partials, "tp", scatter_dimension=1, tiled=True)
    branch = lax.psum_scatter(columns, "fs", scatter_dimension=0, tiled=True)
    return (resid.astype(jnp.float32) + branch.astype(jnp.float32)).astype(jnp.bfloat16)


MESH = pl.DeviceIdType.MESH


PARTS = dict(out=2, up=2, down=2, rows=2)

SCRIPTS = {
    (0, 0): [
        10, 11, 900, 210, 310, 211, 1000, 311, 120, 320, 131, 321, 430, 121, 130, 610, 110, 530, 330, 111,
        331, 431, 1100, 620, 630, 1800, 1310, 1400, 1311, 531, 1600, 1410, 410, 411, 1510, 1610, 420, 1511,
        1611, 1520, 230, 1601, 421, 231, 220, 221, 1620, 1621, 1521, 1530, 1200, 710, 720, 730, 1700, 1900,
        1710, 1910, 1720, 1920, 1531, 1999, 2020, 830, 2023, 2010, 2013, 1630, 2123, 1999, 2000, 1999, 2120,
        2199, 2003, 2110, 520, 2199, 2099, 2099, 2199, 2099, 2100, 521, 1631, 1730, 2199, 1930, 2030, 2130,
        2033, 2133, 510, 820, 2032, 2022, 2012, 2113, 2103, 2199, 511, 2132, 2122, 2002, 2299, 2112, 2102,
        810, 2011, 2031, 2021, 2001, 2131, 2121, 2111, 2230, 2101, 2220, 2210, 2299, 2300,
    ],
    (0, 1): [
        900, 10, 11, 211, 210, 1000, 230, 130, 310, 321, 320, 311, 120, 330, 121, 620, 231, 331, 131, 430,
        110, 431, 1100, 610, 630, 1800, 1310, 1400, 1311, 421, 420, 1410, 1600, 111, 1510, 720, 410, 411,
        1601, 1511, 1610, 1520, 1200, 710, 730, 1700, 1900, 1999, 1999, 1999, 2000, 2099, 2099, 2099, 1521,
        1611, 1710, 2199, 1910, 1620, 2010, 530, 1530, 1621, 1720, 531, 1920, 2100, 2199, 2020, 1630, 1531,
        2120, 2110, 830, 2003, 2023, 2199, 2013, 2103, 221, 220, 510, 2113, 1631, 1730, 1930, 511, 2033, 2123,
        2030, 2130, 520, 810, 2031, 2001, 2021, 2199, 2133, 2199, 2131, 2101, 2011, 2299, 2121, 521, 2111,
        820, 2022, 2032, 2002, 2012, 2132, 2102, 2122, 2230, 2112, 2220, 2210, 2299, 2300,
    ],
    (1, 0): [
        20, 21, 0, 900, 1, 300, 320, 1000, 301, 321, 330, 500, 130, 331, 131, 501, 430, 100, 431, 101, 600,
        620, 630, 1100, 1800, 1300, 1400, 1301, 1320, 1321, 1410, 1610, 1611, 120, 1520, 400, 121, 401, 1521,
        1620, 1500, 420, 1621, 1501, 1600, 1530, 220, 1601, 1531, 1630, 1631, 221, 421, 520, 730, 1200, 1710,
        700, 720, 1910, 1700, 1900, 230, 521, 1720, 1920, 1730, 1930, 800, 820, 2030, 2031, 2010, 231, 200,
        201, 2020, 2110, 1999, 2011, 1999, 2130, 2199, 2032, 2199, 2111, 2012, 2021, 2120, 2000, 2121, 2131,
        1999, 2099, 2132, 2001, 2100, 2002, 2022, 2099, 2199, 2199, 2112, 2122, 2101, 2099, 2200, 2102, 531,
        530, 830, 2199, 2023, 2033, 2013, 2003, 2133, 2113, 2123, 2299, 2103, 2230, 2220, 2299, 2300,
    ],
    (1, 1): [
        20, 900, 0, 1, 21, 300, 320, 1000, 301, 321, 330, 331, 1100, 500, 501, 430, 100, 431, 600, 101, 620,
        630, 1800, 1320, 1400, 1301, 1321, 1410, 1610, 120, 1300, 1520, 400, 130, 1611, 1521, 1500, 420, 1620,
        1501, 421, 401, 1621, 1600, 1530, 131, 1601, 121, 1630, 730, 220, 1531, 1200, 700, 720, 1710, 1910,
        1700, 1900, 1720, 1920, 1631, 1999, 2001, 800, 221, 2000, 2021, 1730, 2099, 2100, 1930, 2099, 230,
        1999, 2199, 2121, 200, 2031, 2199, 2101, 2020, 2030, 2199, 2011, 2131, 2199, 1999, 2010, 2130, 2099,
        2111, 201, 231, 530, 531, 520, 521, 830, 2003, 2023, 2033, 2120, 2199, 2110, 2103, 2123, 2013, 2299,
        2133, 2113, 820, 2032, 2002, 2022, 2012, 2102, 2122, 2132, 2299, 2112, 2230, 2200, 2220, 2300,
    ],
}


GROUPS = dict(z=0, x=1, mixed=1, y=2, c=2, d=2, sum_c=3, sum_y=4, sum_a=5, sum_z=5, gain=6)


def slot_table(fs):
    table, count = {}, 0
    sizes = dict(mixed=3, gain=1, sum_c=2 * fs, sum_y=2 * fs, sum_a=4, sum_z=4, rows_c=fs, rows_d=fs)
    for name, parts in PARTS.items():
        sizes[name + "_z"] = fs * parts
        if name == "rows":
            sizes["rows_y"] = fs * parts
        else:
            sizes[name + "_x"] = fs
    for name, size in sizes.items():
        table[name] = count
        count += size
    return table, count


LETTERS, TWO, ONE = "AUDaudxvzmnlgBybrwPHCFOE", "AUDaudBbrCF", "xvzywHO"


def unpack(code):
    kind, rest = LETTERS[code // 100], code % 100
    if rest == 99:
        return kind, None
    count = 2 if kind in TWO else 1 if kind in ONE else 0
    return kind, [rest // 10, rest % 10][:count]


def segments(script):
    parts, steps = [[]], []
    for token in map(unpack, script):
        if token[0] in "PHCFOE":
            steps.append(token)
            parts.append([])
        else:
            parts[-1].append(token)
    return parts, steps


def layer_kernel(
    fs, slots,
    stream_ref, mixed_ref, out_ref, gain_ref, up_ref, down_ref, result_ref,
    mixw, gains, wo, wup, wdn, rows, acts, kept, send_c, got_c, send_y, got_y, send_z, got_a, got_z,
    held, send_sem, recv_sem, local_sem,
):
    f32, bf16 = jnp.float32, jnp.bfloat16
    g, i, j = lax.axis_index("grp"), lax.axis_index("fs"), lax.axis_index("tp")
    y, c = j // 2, j % 2
    jc = y * 2 + (1 - c)
    jy = (1 - y) * 2 + c
    jd = (1 - y) * 2 + (1 - c)
    half, width = wo.shape[2], wo.shape[3]

    low = i < fs // 2
    v = jnp.where(low, i, fs - 1 - i)
    yr = jnp.where(low, y, 1 - y)
    cr = jnp.where(low, c, 1 - c)

    def real(w):
        return jnp.where(low, w, fs - 1 - w)

    core, across, diag, twin = (g, i, jc), (g, i, jy), (g, i, jd), (1 - g, i, j)
    both = jnp.logical_and

    def at(w):
        return (g, real(w), j)

    def group(name):
        return GROUPS[name] if name in GROUPS else GROUPS[name.split("_")[1]]

    def copy(name, src, dst, target, rk):
        return pltpu.make_async_remote_copy(
            src_ref=src, dst_ref=dst,
            send_sem=send_sem.at[group(name)], recv_sem=recv_sem.at[slots[name] + rk],
            device_id=target, device_id_type=MESH,
        )

    def send(name, src, dst, target, rk):
        copy(name, src, dst, target, rk).start()

    def arrive(name, rk, dst):
        copy(name, dst, dst, core, rk).wait_recv()

    barrier = pltpu.get_barrier_semaphore()
    greeted = [core, across, diag, twin]
    for device in greeted:
        pl.semaphore_signal(barrier, inc=1, device_id=device, device_id_type=MESH)
    for s in range(1, fs):
        pl.semaphore_signal(barrier, inc=1, device_id=(g, lax.rem(i + s, fs), j), device_id_type=MESH)

    def keep(src, dst):
        pltpu.make_async_copy(src, dst, local_sem.at[0]).start()

    def up_piece(owner, part):
        return up_ref.at[pl.ds(part * half, half), pl.ds(pl.multiple_of(owner * width, width), width)]

    def down_piece(owner, part):
        return down_ref.at[pl.ds(owner * 2 * half + part * half, half), :]

    for part in range(2):
        keep(out_ref.at[pl.ds(part * half, half), :], wo.at[i, part])
        keep(up_piece(i, part), wup.at[i, part])
        keep(down_piece(i, part), wdn.at[i, part])
    keep(mixed_ref, mixw.at[j])
    keep(stream_ref, held)
    gains[j] = gain_ref[...].astype(f32).reshape(1, width).astype(bf16)
    pl.semaphore_wait(barrier, len(greeted) + fs - 1)

    def piece(name, ref, q):
        size = ref.shape[0] // PARTS[name]
        return ref.at[pl.ds(q * size, size), :]

    def block_of(name, w):
        if name == "rows":
            return rows.at[j, real(w)]
        return dict(out=wo, up=wup, down=wdn)[name].at[real(w), g]

    def slot(name, b, q):
        return real(b) * PARTS[name] + q

    def pass_on(name, b, q, to):
        block = piece(name, block_of(name, b), q)
        send(name + "_z", block, block, at(to), slot(name, b, q))

    def crossing(b, q):
        block = piece("rows", block_of("rows", b), q)
        send("rows_y", block, block, across, slot("rows", b, q))
        send("rows_c", block, block, core, real(b))

    def twin_copy(name, b, q):
        block = piece(name, block_of(name, b), q)
        send(name + "_x", block, block, twin, real(b))

    def act(own, token):
        kind, args = token
        if kind in "AUD":
            w, q = args
            name = dict(A="out", U="up", D="down")[kind]
            to = real(w)
            source = dict(
                A=out_ref.at[pl.ds(g * half, half), :], U=up_piece(to, g), D=down_piece(to, g)
            )[kind]
            send(
                name + "_z", piece(name, source, q), piece(name, block_of(name, own), q), at(w),
                slot(name, own, q),
            )
        elif kind in "aud":
            b, q = args
            name = dict(a="out", u="up", d="down")[kind]
            arrive(name + "_z", slot(name, b, q), piece(name, block_of(name, b), q))
            if kind == "a":
                to = own + 1 if b < own else own - 1
                if to >= 0:
                    pass_on(name, b, q, to)
            twin_copy(name, b, q)
        elif kind in "xvz":
            (b,) = args
            name, buffer = dict(x=("out", wo), v=("up", wup), z=("down", wdn))[kind]
            arrive(name + "_x", real(b), buffer.at[real(b), 1 - g])
        elif kind == "m":
            send("mixed", mixed_ref, mixw.at[j], across, 0)
            send("mixed", mixed_ref, mixw.at[j], core, 1)
            for target in (across, core, diag):
                send("gain", gains.at[j], gains.at[j], target, 0)
        elif kind == "n":
            arrive("mixed", 0, mixw.at[jy])
            send("mixed", mixw.at[jy], mixw.at[jy], core, 2)
        elif kind == "l":
            arrive("mixed", 1, mixw.at[jc])
            arrive("mixed", 2, mixw.at[jd])
        elif kind == "g":
            arrive("gain", 0, gains.at[pl.ds(0, 3)])
        elif kind == "B":
            w, q = args
            pass_on("rows", own, q, w)
        elif kind == "y":
            (q,) = args
            crossing(own, q)
        elif kind == "b":
            b, q = args
            arrive("rows_z", slot("rows", b, q), piece("rows", block_of("rows", b), q))
            to = own + 1 if b < own else own - 1
            if to >= 0:
                pass_on("rows", b, q, to)
            crossing(b, q)
        elif kind == "r":
            b, q = args
            block = piece("rows", rows.at[jy, real(b)], q)
            arrive("rows_y", slot("rows", b, q), block)
            send("rows_d", block, block, core, real(b))
        elif kind == "w":
            (b,) = args
            arrive("rows_c", real(b), rows.at[jc, real(b)])
            arrive("rows_d", real(b), rows.at[jd, real(b)])

    def whole(ref, k):
        return ref[k].reshape(2 * half, width)

    kinds = [(a, b) for a in range(2) for b in range(2)]
    plans = [segments(SCRIPTS[kind]) for kind in kinds]

    def pick(values):
        lower = values[0] if values[0] == values[1] else jnp.where(yr == 0, values[0], values[1])
        upper = values[2] if values[2] == values[3] else jnp.where(yr == 0, values[2], values[3])
        if list(values[:2]) == list(values[2:]):
            return lower
        return jnp.where(v == 0, lower, upper)

    def project():
        pltpu.make_async_copy(send_c, got_c, local_sem.at[0]).wait()
        total = held[...].astype(f32)
        for k in range(fs):
            total += jnp.dot(mixw[k], whole(wo, k), preferred_element_type=f32)
        rows[j, i] = total.astype(bf16)

    def hidden(t):
        z = real(t)
        wide = [rows[k, z].astype(f32) for k in range(rows.shape[0])]
        energy = sum(jnp.sum(w * w, axis=1, keepdims=True) for w in wide)
        scale = lax.rsqrt(energy * (1.0 / (len(wide) * width)) + epsilon)
        up = None
        for k, w in enumerate(wide):
            normed = (w * scale * gains[k].astype(f32)).astype(bf16)
            term = jnp.dot(normed, whole(wup, k), preferred_element_type=f32)
            up = term if up is None else up + term
        acts[t] = jnp.square(jnp.maximum(up, 0.0)).astype(bf16)

    def column(t, k):
        p = k // 2
        part = jnp.dot(acts[t], whole(wdn, real(k)), preferred_element_type=f32)

        @pl.when(k % 2 != cr)
        def _():
            send_c[p, t] = part.astype(bf16)
            copy("sum_c", send_c.at[p, t], got_c.at[p, t], core, p * fs + t).start()

        @pl.when(k % 2 == cr)
        def _():
            kept[p, t] = part

    tokens = held.shape[0]
    spans = [pl.ds(h * (tokens // 2), tokens // 2) for h in range(2)]

    def fold(t, k):
        p = k // 2

        @pl.when(k % 2 == cr)
        def _():
            arrive("sum_c", p * fs + t, got_c.at[p, t])

            @pl.when(p != yr)
            def _():
                for h, span in enumerate(spans):
                    send_y[t, span] = (kept[p, t, span] + got_c[p, t, span].astype(f32)).astype(bf16)
                    copy("sum_y", send_y.at[t, span], got_y.at[t, span], across, 2 * t + h).start()

            @pl.when(p == yr)
            def _():
                kept[p, t] = kept[p, t] + got_c[p, t].astype(f32)

    def offer(t):
        e = t - fs // 2
        for h, span in enumerate(spans):
            arrive("sum_y", 2 * t + h, got_y.at[t, span])

            @pl.when(both(v == 1, t >= fs // 2))
            def _():
                arrive("sum_a", 2 * e + h, got_a.at[e, span])
                part = kept[yr, t, span] + got_y[t, span].astype(f32) + got_a[e, span].astype(f32)
                send_z[t, span] = part.astype(bf16)
                copy("sum_z", send_z.at[t, span], got_z.at[1, span], at(t), 2 + h).start()

            @pl.when(both(v == 0, t >= fs // 2))
            def _():
                send_z[t, span] = (kept[yr, t, span] + got_y[t, span].astype(f32)).astype(bf16)
                copy("sum_a", send_z.at[t, span], got_a.at[e, span], at(1), 2 * e + h).start()

            @pl.when(t < fs // 2)
            def _():
                send_z[t, span] = (kept[yr, t, span] + got_y[t, span].astype(f32)).astype(bf16)
                copy("sum_z", send_z.at[t, span], got_z.at[0, span], at(t), h).start()

    def finish():
        for h, span in enumerate(spans):
            arrive("sum_y", 2 * v + h, got_y.at[v, span])
            branch = kept[yr, v, span] + got_y[v, span].astype(f32)
            for n in range(2):
                arrive("sum_z", 2 * n + h, got_z.at[n, span])
                branch += got_z[n, span].astype(f32)
            held[span] = (rows[j, i, span].astype(f32) + branch).astype(bf16)

    mine = [v == own for own in range(2)]
    exact = [[both(mine[own], yr == b) for b in range(2)] for own in range(2)]
    for n in range(len(plans[0][0])):
        for own in range(2):
            lists = [plans[2 * own + b][0][n] for b in range(2)]
            if lists[0] == lists[1]:
                if lists[0]:
                    @pl.when(mine[own])
                    def _():
                        for token in lists[0]:
                            act(own, token)
            else:
                for b in range(2):
                    if lists[b]:
                        given = exact[own][b]

                        @pl.when(given)
                        def _():
                            for token in lists[b]:
                                act(own, token)
        if n < len(plans[0][1]):
            steps = [plan[1][n] for plan in plans]
            kind = steps[0][0]
            taken = [step[1] is not None for step in steps]
            if not any(taken):
                continue
            default = steps[taken.index(True)]
            choices = [step[1] if used else default[1] for step, used in zip(steps, taken)]
            args = [pick(list(values)) for values in zip(*choices)]
            run = dict(P=project, H=hidden, C=column, F=fold, O=offer, E=finish)[kind]
            if all(taken):
                run(*args)
            else:
                here = functools.reduce(
                    jnp.logical_or, [one for one, used in zip(exact[0] + exact[1], taken) if used]
                )
                pl.when(here)(functools.partial(run, *args))

    out_copy = pltpu.make_async_copy(held, result_ref, local_sem.at[1])
    out_copy.start()

    def drain(name, total):
        copy(name, total, total, core, 0).wait_send()

    @pl.when(v == 0)
    def _():
        drain("out_z", got_c)

    @pl.when(v == 1)
    def _():
        drain("out_z", rows)

    drain("mixed", rows.at[pl.ds(0, 3)])
    drain("rows_y", rows.at[pl.ds(0, 3)])
    drain("sum_c", got_c)
    drain("sum_y", got_y)
    drain("sum_z", send_z.at[pl.ds(0, 3)])
    drain("gain", gains.at[pl.ds(0, 3)])
    out_copy.wait()


def kernel_body(fs, tp, stream, mixed, out_weight, norm_gain, up_weight, down_weight):
    tokens, width = stream.shape
    half = out_weight.shape[0] // 2
    slots, count = slot_table(fs)
    vmem, anywhere = pl.BlockSpec(memory_space=pltpu.VMEM), pl.BlockSpec(memory_space=pl.ANY)
    weights = pltpu.VMEM((fs, 2, half, width), jnp.bfloat16)
    blocks = pltpu.VMEM((fs, tokens, width), jnp.bfloat16)
    columns = pltpu.VMEM((2, fs, tokens, width), jnp.bfloat16)
    pair = pltpu.VMEM((2, tokens, width), jnp.bfloat16)
    return pl.pallas_call(
        functools.partial(layer_kernel, fs, slots),
        out_shape=jax.ShapeDtypeStruct((tokens, width), jnp.bfloat16),
        in_specs=[anywhere, anywhere, anywhere, vmem, anywhere, anywhere],
        out_specs=anywhere,
        scratch_shapes=[
            pltpu.VMEM((tp, tokens, width), jnp.bfloat16),
            pltpu.VMEM((tp, 1, width), jnp.bfloat16),
            weights, weights, weights,
            pltpu.VMEM((tp, fs, tokens, width), jnp.bfloat16),
            blocks,
            pltpu.VMEM((2, fs, tokens, width), jnp.float32),
            columns, columns, blocks, blocks, blocks, pair, pair,
            pltpu.VMEM((tokens, width), jnp.bfloat16),
            pltpu.SemaphoreType.DMA((7,)),
            pltpu.SemaphoreType.DMA((count,)),
            pltpu.SemaphoreType.DMA((2,)),
        ],
        compiler_params=pltpu.CompilerParams(
            collective_id=0, has_side_effects=True, vmem_limit_bytes=56 * 1024 * 1024
        ),
    )(stream, mixed, out_weight, norm_gain, up_weight, down_weight)


def solution(mesh):
    placed = (
        P(("grp", "fs"), "tp"),
        P(("grp", "fs"), "tp"),
        P("fs", "tp"),
        P("tp"),
        P("fs", "tp"),
        P("tp", "fs"),
    )
    fs, tp = mesh.shape["fs"], mesh.shape["tp"]

    def call(stream, mixed, out_weight, norm_gain, up_weight, down_weight):
        width, hidden = up_weight.shape
        tokens = stream.shape[0] // mesh.shape["grp"]
        moved_weights = 2 * width * hidden // tp
        moved_rows = 2 * tokens * width + 2 * width * hidden // (tp * fs)
        aligned = fs == tp == 4 and (width // tp) % 256 == 0 and (tokens // fs) % 16 == 0
        aligned = aligned and hidden == tp * width
        body = spread_body if moved_rows < moved_weights else gathered_body
        if aligned and moved_rows < moved_weights:
            body = functools.partial(kernel_body, fs, tp)
        return sharded(body)(stream, mixed, out_weight, norm_gain, up_weight, down_weight)

    def sharded(body):
        return jax.shard_map(
            body, mesh=mesh, in_specs=placed, out_specs=P(("grp", "fs"), "tp"), check_vma=False
        )

    return call
```
